256 devices in a mesh: rep: 2 (over z_hi), fs: 16 (over z_lo, x), tp: 8 (over y, core).
Axes of the slice: x: 4, y: 4, z: 8 (z_hi: 2, z_lo: 4; z = z_hi * 4 + z_lo), core: 2. Of those that a mesh axis runs over, the one named last changes fastest.
Arguments:
- tokens: bfloat16 [16384, 2048], P(('rep', 'fs'), 'tp'), may hold values from -7 to 7
- norm_gain: float32 [2048], P('tp'), may hold values from 0.1 to 1.9
- value_weight: bfloat16 [2048, 512], P('fs', 'tp'), may hold values from -0.125 to 0.125
- glu_weight: bfloat16 [2048, 512], P('fs', 'tp'), may hold values from -0.125 to 0.125
- conv_kernel: bfloat16 [31, 512], P(None, 'tp'), may hold values from -1.5 to 1.5
- conv_gain: float32 [512], P('tp'), may hold values from 0.1 to 1.9
- proj_weight: bfloat16 [512, 2048], P('fs', 'tp'), may hold values from -0.25 to 0.25
- mlp_gain: float32 [2048], P('tp'), may hold values from 0.1 to 1.9
- gate_weight: bfloat16 [2048, 5632], P('fs', 'tp'), may hold values from -0.125 to 0.125
- up_weight: bfloat16 [2048, 5632], P('fs', 'tp'), may hold values from -0.125 to 0.125
- down_weight: bfloat16 [5632, 2048], P('tp', 'fs'), may hold values from -0.078125 to 0.078125
- out_gain: float32 [2048], P('tp'), may hold values from 0.1 to 1.9
Outputs:
- layer_out: bfloat16 [16384, 2048], P(('rep', 'fs'), 'tp')
The draws below stay inside these ranges and needn't reach their ends.
All inputs are finite; a program needn't handle non-finite values.
Results may differ from the reference program's by a relative error of at most 0.0085.
Values may be sent and summed in bfloat16 or wider, within the bound.
No kernel may reach another device: no remote copies, remote signals or barrier semaphores. Data moves between devices by JAX's collectives and lax.ppermute only.
A program may use at most 64 MiB of HBM per device.

```python
import jax
import jax.numpy as jnp
from jax import lax

D = 2048
CONV = 512
FF = 5632
TAPS = 31
SEQ_LEN = 256
TOKENS = 16384
N_TP = 8


def ladder(key, count):
    order = jax.random.permutation(key, count).astype(jnp.float32)
    return 3.0 ** (order / max(count - 1, 1) - 0.5)


def draw_tokens(key, part):
    scales = jnp.repeat(ladder(jax.random.fold_in(key, 11), N_TP), D // N_TP)
    base = jnp.clip(jax.random.normal(jax.random.fold_in(key, 14), (TOKENS, D), jnp.float32), -4.0, 4.0)
    values = base * scales
    return values.astype(jnp.bfloat16)


def draw_conv_kernel(key, part):
    scales = jnp.repeat(ladder(jax.random.fold_in(key, 21), N_TP), CONV // N_TP)
    base = jnp.clip(jax.random.normal(jax.random.fold_in(key, 23), (TAPS, CONV), jnp.float32), -4.0, 4.0)
    values = base * scales * TAPS ** (-0.5)
    return values.astype(jnp.bfloat16)


def levels(key, extent, shards, smallest, high):
    loudness = 1.0
    for axis_at, parts in shards:
        draws = jax.random.uniform(jax.random.fold_in(jax.random.fold_in(key, 6), axis_at), (parts,), jnp.float32, smallest / len(shards), high / len(shards))
        loudness = loudness * jnp.repeat(jnp.exp(draws), extent[axis_at] // parts).reshape((-1,) + (1,) * (len(extent) - 1 - axis_at))
    return loudness


def scatter_about(own_key, extent, scale, most, pieces=(), held_as=jnp.bfloat16):
    loudness = levels(own_key, extent, pieces, -0.22, 0.18) if pieces else 1.0
    entries = jax.random.normal(own_key, extent, jnp.float32) * scale * loudness
    return jnp.minimum(jnp.maximum(entries, -most), most).astype(held_as)


def setup_inputs(seed: int = 0) -> dict:
    streams_of = jax.random.split(jax.random.key(seed), 13)
    tokens = draw_tokens(jax.random.fold_in(streams_of[12], 71), 0)
    norm_gain = jnp.clip(1.0 + 0.18 * jax.random.normal(streams_of[1], (D,), jnp.float32), 0.1, 1.9)
    value_weight = scatter_about(streams_of[2], (D, CONV), D ** -0.5, 0.125, ((0, 16), (1, 8)))
    glu_weight = scatter_about(streams_of[3], (D, CONV), D ** -0.5, 0.125, ((0, 16), (1, 8)))
    conv_kernel = draw_conv_kernel(jax.random.fold_in(streams_of[12], 71), 0)
    conv_gain = jnp.clip(1.0 + 0.18 * jax.random.normal(streams_of[5], (CONV,), jnp.float32), 0.1, 1.9)
    proj_weight = scatter_about(streams_of[6], (CONV, D), CONV ** -0.5, 0.25, ((0, 16), (1, 8)))
    mlp_gain = jnp.clip(1.0 + 0.18 * jax.random.normal(streams_of[7], (D,), jnp.float32), 0.1, 1.9)
    gate_weight = scatter_about(streams_of[8], (D, FF), D ** -0.5, 0.125, ((0, 16), (1, 8)))
    up_weight = scatter_about(streams_of[9], (D, FF), D ** -0.5, 0.125, ((0, 16), (1, 8)))
    down_weight = scatter_about(streams_of[10], (FF, D), FF ** -0.5, 0.078125, ((0, 8), (1, 16)))
    out_gain = jnp.clip(1.0 + 0.18 * jax.random.normal(streams_of[11], (D,), jnp.float32), 0.1, 1.9)
    return {"tokens": tokens, "norm_gain": norm_gain, "value_weight": value_weight, "glu_weight": glu_weight, "conv_kernel": conv_kernel, "conv_gain": conv_gain, "proj_weight": proj_weight, "mlp_gain": mlp_gain, "gate_weight": gate_weight, "up_weight": up_weight, "down_weight": down_weight, "out_gain": out_gain}


EPS = 1e-05

def layer_norm(values, gain):
    mean = lax.optimization_barrier(jnp.mean(values, axis=-1, keepdims=True))
    var = lax.optimization_barrier(jnp.mean(jnp.square(values - mean), axis=-1, keepdims=True))
    return (values - mean) * lax.rsqrt(var + EPS) * gain.astype(jnp.float32)

def reference(tokens, norm_gain, value_weight, glu_weight, conv_kernel, conv_gain, proj_weight, mlp_gain, gate_weight, up_weight, down_weight, out_gain):
    start = tokens.astype(jnp.float32)
    hin = layer_norm(start, norm_gain).astype(jnp.bfloat16)
    values = jnp.dot(hin, value_weight, preferred_element_type=jnp.float32).astype(jnp.bfloat16)
    glus = jnp.dot(hin, glu_weight, preferred_element_type=jnp.float32).astype(jnp.bfloat16)
    values, glus = lax.optimization_barrier((values, glus))
    unit = values.astype(jnp.float32) * jax.nn.sigmoid(glus.astype(jnp.float32))
    count = unit.shape[0] // SEQ_LEN
    unit = unit.reshape(count, SEQ_LEN, unit.shape[1])
    padded = jnp.pad(unit, ((0, 0), (TAPS - 1, 0), (0, 0)))
    kernel = conv_kernel.astype(jnp.float32)
    conv = jnp.zeros_like(unit)
    for shift in range(TAPS):
        conv = conv + kernel[shift] * padded[:, TAPS - 1 - shift:TAPS - 1 - shift + SEQ_LEN]
    conv = conv.reshape(count * SEQ_LEN, conv.shape[2])
    mixed = jax.nn.silu(layer_norm(conv, conv_gain)).astype(jnp.bfloat16)
    first = start + jnp.dot(mixed, proj_weight, preferred_element_type=jnp.float32)
    hmid = layer_norm(first, mlp_gain).astype(jnp.bfloat16)
    gates = jnp.dot(hmid, gate_weight, preferred_element_type=jnp.float32)
    ups = jnp.dot(hmid, up_weight, preferred_element_type=jnp.float32)
    hidden = (jax.nn.silu(gates) * ups).astype(jnp.bfloat16)
    block = FF // N_TP
    second = first
    for index in range(N_TP):
        part_sum = jnp.dot(hidden[:, index * block:(index + 1) * block], down_weight[index * block:(index + 1) * block], preferred_element_type=jnp.float32)
        part_sum = lax.optimization_barrier(part_sum.astype(jnp.bfloat16))
        second = second + part_sum.astype(jnp.float32)
    return layer_norm(second, out_gain).astype(jnp.bfloat16)
```

```python
import jax
import jax.numpy as jnp
from jax import lax
from jax.sharding import Mesh
from jax.sharding import PartitionSpec as P


SEQ_LEN = 256
EPS = 1e-05
Z = ("rep", "z")
BF = jnp.bfloat16
F32 = jnp.float32
CUT = 640
DCUT = 288


def from_ring(x, axes, step, size):
    return lax.ppermute(x, axes, [((i + step) % size, i) for i in range(size)])


def x_from(x, step):
    return from_ring(x, "x", step, 4)


def y_from(x, step):
    return from_ring(x, "y", step, 4)


def z_from(x, step):
    if step == 2:
        return lax.ppermute(x, Z, [((i + (2 if i % 2 == 0 else -2)) % 8, i) for i in range(8)])
    return from_ring(x, Z, step, 8)


def swap(x):
    return lax.ppermute(x, "core", [(0, 1), (1, 0)])


def direct(x, get):
    return [x, get(x, 1), get(x, 2), get(x, -1)]


def relayed(x, get, dim):
    after, before = get(x, 1), get(x, -1)
    half = x.shape[dim] // 2
    low = get(lax.slice_in_dim(after, 0, half, axis=dim), 1)
    high = get(lax.slice_in_dim(before, half, 2 * half, axis=dim), -1)
    return [x, after, (low, high), before]


def in_order(pieces, at):
    both = jnp.stack(pieces + pieces)
    return lax.dynamic_slice_in_dim(both, (4 - at) % 4, 4, axis=0)


def lanes(stacked):
    return jnp.concatenate([stacked[i] for i in range(stacked.shape[0])], axis=-1)


def by_core(core, mine, other, axis=-1):
    return jnp.where(
        core == 0,
        jnp.concatenate([mine, other], axis=axis),
        jnp.concatenate([other, mine], axis=axis),
    )


def in_three(g):
    high = g.astype(BF)
    rest = g - high.astype(F32)
    mid = rest.astype(BF)
    return [high, mid, (rest - mid.astype(F32)).astype(BF)]


def norm(values, gain):
    width = values.shape[-1]
    mean = jnp.sum(values, axis=-1, keepdims=True) / width
    off = values - mean
    var = jnp.sum(off * off, axis=-1, keepdims=True) / width
    return off * lax.rsqrt(var + EPS) * gain


def dot(a, b):
    return jnp.dot(a, b, preferred_element_type=F32)


def per_device(
    tokens,
    norm_gain,
    value_weight,
    glu_weight,
    conv_kernel,
    conv_gain,
    proj_weight,
    mlp_gain,
    gate_weight,
    up_weight,
    down_weight,
    out_gain,
):
    x, y, core = lax.axis_index("x"), lax.axis_index("y"), lax.axis_index("core")
    z = lax.axis_index("z")
    half = SEQ_LEN

    params = []
    for g in (norm_gain, mlp_gain, out_gain, jnp.pad(conv_gain, (0, 192))):
        params += in_three(g)
    params = jnp.stack(params + [jnp.zeros((256,), BF)] * 4)
    mine = lax.dynamic_slice_in_dim(tokens, core * half, half, axis=0)
    theirs = lax.dynamic_slice_in_dim(tokens, (1 - core) * half, half, axis=0)
    got = swap(jnp.concatenate([theirs, params]))
    pair = by_core(core, jnp.concatenate([mine, params]), got)
    wide = lanes(in_order(direct(pair, y_from), y))
    start = wide[:half].astype(F32)
    gains = wide[half : half + 12].astype(F32)
    gains = [gains[3 * i] + gains[3 * i + 1] + gains[3 * i + 2] for i in range(4)]
    conv_gain_full = gains[3].reshape(8, 256)[:, :64].reshape(512)
    other_kernel = swap(conv_kernel)
    kernel = by_core(core, conv_kernel, other_kernel).astype(F32)

    small = jnp.concatenate(
        [jnp.concatenate([value_weight, glu_weight], axis=1), proj_weight.reshape(64, 128)]
    )
    row = in_order(direct(small, x_from), x)
    plane = in_order(direct(row, z_from), z).reshape(16, 192, 128)
    vg = plane[:, :128].reshape(2048, 128)
    vg_other = swap(vg)
    value_full = by_core(core, vg[:, :64], vg_other[:, :64])
    glu_full = by_core(core, vg[:, 64:], vg_other[:, 64:])
    proj_cols = plane[:, 128:].reshape(512, 256)
    proj_mine = in_order(direct(proj_cols, y_from), y)
    proj_other = swap(proj_mine)
    proj_full = lanes(by_core(core, proj_mine, proj_other))

    a = jnp.concatenate([gate_weight, up_weight[:, CUT:]], axis=1)
    b = up_weight[:, :CUT]
    da, db = down_weight[:DCUT], down_weight[DCUT:]
    a_row = in_order(direct(a, x_from), x).reshape(512, a.shape[1])
    b_col = in_order(direct(b, z_from), z).reshape(512, b.shape[1])
    da_row = lanes(in_order(direct(da, x_from), x))
    db_col = lanes(in_order(direct(db, z_from), z))
    a_all = relayed(a_row, z_from, 0)
    b_all = relayed(b_col, x_from, 0)
    da_all = relayed(da_row, z_from, 0)
    db_all = relayed(db_col, x_from, 0)

    hin = norm(start, gains[0]).astype(BF)
    values, glus = lax.optimization_barrier(
        (dot(hin, value_full).astype(BF), dot(hin, glu_full).astype(BF))
    )
    unit = values.astype(F32) * jax.nn.sigmoid(glus.astype(F32))
    taps = kernel.shape[0]
    padded = jnp.pad(unit, ((taps - 1, 0), (0, 0)))
    conv = jnp.zeros_like(unit)
    for shift in range(taps):
        conv = conv + kernel[shift] * padded[taps - 1 - shift : taps - 1 - shift + half]
    conv_full = lanes(in_order(direct(conv.astype(BF), y_from), y)).astype(F32)
    mixed = jax.nn.silu(norm(conv_full, conv_gain_full)).astype(BF)
    first = start + dot(mixed, proj_full)
    hmid_mine = norm(first, gains[1]).astype(BF)
    hmid = by_core(core, hmid_mine, swap(hmid_mine), axis=0)

    by_z = hmid.reshape(512, 4, 512)
    by_x = hmid.reshape(512, 4, 4, 128).transpose(2, 0, 1, 3).reshape(4, 512, 512)

    def summed(pieces, at, take):
        total = 0
        for k in (0, 1, 3, 2):
            left = take((at + k) % 4)
            if isinstance(pieces[k], tuple):
                h = pieces[k][0].shape[0]
                total = total + dot(left[:, :h], pieces[k][0]) + dot(left[:, h:], pieces[k][1])
            else:
                total = total + dot(left, pieces[k])
        return total

    at_z = lambda j: lax.dynamic_slice_in_dim(by_z, j, 1, axis=1)[:, 0]
    at_x = lambda j: lax.dynamic_slice_in_dim(by_x, j, 1, axis=0)[0]
    ga = summed(a_all, z, at_z)
    gb = summed(b_all, x, at_x)
    gates = ga[:, :704]
    ups = jnp.concatenate([gb, ga[:, 704:]], axis=1)
    hidden = (jax.nn.silu(gates) * ups).astype(BF)

    def whole(p):
        return jnp.concatenate(p, axis=0) if isinstance(p, tuple) else p

    down_a = lanes(in_order([whole(p) for p in da_all], z))
    down_b = in_order([whole(p) for p in db_all], x)
    down_b = down_b.reshape(4, 704 - DCUT, 4, 128).transpose(1, 2, 0, 3).reshape(704 - DCUT, 2048)
    part = dot(hidden, jnp.concatenate([down_a, down_b], axis=0)).astype(BF)
    keep = lax.dynamic_slice_in_dim(part, core * half, half, axis=0)
    give = lax.dynamic_slice_in_dim(part, (1 - core) * half, half, axis=0)
    chip = keep.astype(F32) + swap(give).astype(F32)

    def cols(v, at):
        return lax.dynamic_slice_in_dim(v, (at % 4) * 512, 512, axis=1)

    second = cols(first, y) + cols(chip, y)
    for k in (2, 1, 3):
        sent = cols(chip, y - k).astype(BF)
        second = second + y_from(sent, k).astype(F32)
    sums = jnp.stack([jnp.sum(second, axis=1), jnp.sum(second * second, axis=1)])
    total = sums
    for k in (2, 1, 3):
        total = total + y_from(sums, k)
    mean = (total[0] / 2048)[:, None]
    var = (total[1] / 2048)[:, None] - mean * mean
    gain = lax.dynamic_slice_in_dim(gains[2], y * 512, 512, axis=0)
    out = ((second - mean) * lax.rsqrt(var + EPS) * gain).astype(BF)
    keep = lax.dynamic_slice_in_dim(out, core * 256, 256, axis=1)
    give = lax.dynamic_slice_in_dim(out, (1 - core) * 256, 256, axis=1)
    return by_core(core, keep, swap(give), axis=0)


def solution(mesh):
    split = Mesh(
        mesh.devices.reshape(2, 4, 4, 4, 2), ("rep", "z", "x", "y", "core")
    )
    rows, fs, tp = ("rep", "z", "x"), ("z", "x"), ("y", "core")
    in_specs = (
        P(rows, tp),
        P(tp),
        P(fs, tp),
        P(fs, tp),
        P(None, tp),
        P(tp),
        P(fs, tp),
        P(tp),
        P(fs, tp),
        P(fs, tp),
        P(tp, fs),
        P(tp),
    )
    return jax.shard_map(
        per_device, mesh=split, in_specs=in_specs, out_specs=P(rows, tp), check_vma=False
    )
```

```python
import functools

import jax
import jax.numpy as jnp
from jax import lax
from jax.experimental import pallas as pl
from jax.experimental.pallas import tpu as pltpu
from jax.sharding import Mesh
from jax.sharding import PartitionSpec as P


EPS = 1e-05
Z = ("rep", "z")
TP = ("y", "core")
BF = jnp.bfloat16
F32 = jnp.float32
SEQ = 256
TAPS = 31
FF = 704
DA, DB = 192, 512
A_ROWS, B_ROWS = FF + DA, FF + DB
CHUNKS = ((0, 256), (256, 512), (512, 704))
EXTRA = 16


def call(body, outs, args, scratch=(), flops=0):
    size = sum(a.size * a.dtype.itemsize for a in args) + sum(
        functools.reduce(lambda p, q: p * q, s, 1) * jnp.dtype(d).itemsize for s, d in outs
    )
    held = sum(
        functools.reduce(lambda p, q: p * q, s, 1) * jnp.dtype(d).itemsize for s, d in scratch
    )
    return pl.pallas_call(
        body,
        out_shape=[jax.ShapeDtypeStruct(s, d) for s, d in outs],
        in_specs=[pl.BlockSpec(memory_space=pltpu.SMEM)]
        + [pl.BlockSpec(memory_space=pltpu.VMEM)] * (len(args) - 1),
        out_specs=[pl.BlockSpec(memory_space=pltpu.VMEM)] * len(outs),
        scratch_shapes=[pltpu.VMEM(s, d) for s, d in scratch],
        compiler_params=pltpu.CompilerParams(vmem_limit_bytes=size + held + (6 << 20)),
        cost_estimate=pl.CostEstimate(
            flops=max(flops, size * 300), bytes_accessed=size, transcendentals=0
        ),
    )(*args)


def ring(x, axes, step, size):
    return lax.ppermute(x, axes, [((i + step) % size, i) for i in range(size)])


def y_from(x, step):
    return ring(x, "y", step, 4)


def x_from(x, step):
    return ring(x, "x", step, 4)


def z_from(x, step):
    if step == 2:
        return lax.ppermute(x, Z, [((i + (2 if i % 2 == 0 else -2)) % 8, i) for i in range(8)])
    return ring(x, Z, step, 8)


def swap(x):
    return lax.ppermute(x, "core", [(0, 1), (1, 0)])


def exchange(x, axes):
    return lax.all_to_all(x, axes, 0, 0, tiled=True)


def dot(a, b):
    return jnp.dot(a, b, preferred_element_type=F32)


def dot_t(a, b):
    return lax.dot_general(a, b, (((1,), (1,)), ((), ())), preferred_element_type=F32)


def silu(v):
    return v * jax.nn.sigmoid(v)


def pack_tokens(at, tokens, norm_gain, mlp_gain, conv_gain, out_gain, out):
    row = lax.broadcasted_iota(jnp.int32, (EXTRA, 256), 0)
    extra = jnp.zeros((EXTRA, 256), F32)
    wide = jnp.concatenate([conv_gain[...], jnp.zeros((1, 192), F32)], axis=1)
    for i, g in enumerate((norm_gain[...], mlp_gain[...], wide, out_gain[...])):
        high = g.astype(BF).astype(F32)
        mid = (g - high).astype(BF).astype(F32)
        low = g - high - mid
        for j, part in enumerate((high, mid, low)):
            extra = jnp.where(row == 3 * i + j, part, extra)
    extra = extra.astype(BF)
    for t in range(8):
        c = t % 2
        out[t, 0:SEQ] = tokens[c * SEQ : (c + 1) * SEQ]
        out[t, SEQ:] = extra


def gain_of(got, t, i):
    rows = got[t, SEQ:].astype(F32)
    return rows[3 * i : 3 * i + 1] + rows[3 * i + 1 : 3 * i + 2] + rows[3 * i + 2 : 3 * i + 3]


def pack_small(at, value, glu, proj, out):
    out[0:64] = value[...]
    out[64:128] = glu[...]
    out[128:160] = proj[:, 0:128]
    out[160:192] = proj[:, 128:256]


def pack_row(at, s0, s1, s2, s3, out):
    for k, s in enumerate((s0, s1, s2, s3)):
        out[(at[0] + k) % 4] = s[...]


def pack_weights(at, gate, up, down, a, b):
    a[0:FF] = gate[...]
    a[FF:] = down[0:DA]
    b[0:FF] = up[...]
    b[FF:] = down[DA:]


def pack_halves(place):
    def body(at, p0, p1, p2, p3, low, high):
        for k, p in enumerate((p0, p1, p2, p3)):
            i = (at[place] + k) % 4

            @pl.when(i < 2)
            def _():
                low[i] = p[...]

            @pl.when(i >= 2)
            def _():
                high[i - 2] = p[...]

    return body


def pack_plane(at, s0, s1, s2, s3, vg, proj):
    for k, s in enumerate((s0, s1, s2, s3)):
        zz = (at[2] + k) % 4
        for i in range(4):
            vg[zz * 4 + i] = s[i, 0:128]
            for t in range(4):
                proj[t, zz * 4 + i] = s[i, 128:192]


def module_in(at, got, vg, vg_other, taps, taps_other, out, padded):
    core = at[3]
    total = jnp.zeros((SEQ, 1), F32)
    for t in range(8):
        total = total + jnp.sum(got[t, 0:SEQ].astype(F32), axis=1, keepdims=True)
    mean = total / 2048
    total = jnp.zeros((SEQ, 1), F32)
    for t in range(8):
        off = got[t, 0:SEQ].astype(F32) - mean
        total = total + jnp.sum(off * off, axis=1, keepdims=True)
    scale = lax.rsqrt(total / 2048 + EPS)
    acc = jnp.zeros((SEQ, 256), F32)
    for t in range(8):
        hin = ((got[t, 0:SEQ].astype(F32) - mean) * scale * gain_of(got, t, 0)).astype(BF)
        w = jnp.concatenate(
            [jnp.concatenate([v[2 * t], v[2 * t + 1]], axis=1) for v in (vg, vg_other)], axis=0
        )
        acc = acc + dot_t(hin, w)
    both = acc.astype(BF).astype(F32)
    lane = lax.broadcasted_iota(jnp.int32, (SEQ, 128), 1)

    def gated(v):
        return v * jax.nn.sigmoid(pltpu.roll(v, 64, 1))

    mine, other = gated(both[:, 0:128]), gated(both[:, 128:256])
    is0 = core == 0
    unit = jnp.where(
        lane < 64,
        jnp.where(is0, mine, other),
        pltpu.roll(jnp.where(is0, other, mine), 64, 1),
    )
    padded[0:32] = jnp.zeros((32, 128), F32)
    padded[32:] = unit
    ta, tb = taps[...].astype(F32), taps_other[...].astype(F32)
    first, second = jnp.where(is0, ta, tb), jnp.where(is0, tb, ta)
    k = jnp.concatenate([first, second], axis=1)
    conv = jnp.zeros((SEQ, 128), F32)
    for s in range(TAPS):
        conv = conv + k[s : s + 1] * padded[32 - s : 32 - s + SEQ]
    out[...] = conv.astype(BF)


def module_out(at, got, c0, c1, c2, c3, proj, proj_other, hmid, keep, first, mixed):
    y, core = at[1], at[3]
    conv = (c0, c1, c2, c3)
    total = jnp.zeros((SEQ, 1), F32)
    for k in range(4):
        total = total + jnp.sum(conv[k][...].astype(F32), axis=1, keepdims=True)
    mean = total / 512
    total = jnp.zeros((SEQ, 1), F32)
    for k in range(4):
        off = conv[k][...].astype(F32) - mean
        total = total + jnp.sum(off * off, axis=1, keepdims=True)
    scale = lax.rsqrt(total / 512 + EPS)
    for k in range(4):
        t = (y + k) % 4
        gain = jnp.concatenate(
            [gain_of(got, 2 * t, 2)[:, 0:64], gain_of(got, 2 * t + 1, 2)[:, 0:64]], axis=1
        )
        mixed[:, pl.ds(pl.multiple_of(t * 128, 128), 128)] = silu(
            (conv[k][...].astype(F32) - mean) * scale * gain
        ).astype(BF)
    total = jnp.zeros((SEQ, 1), F32)
    for t in range(4):
        for p, c in ((proj, core), (proj_other, 1 - core)):
            w = jnp.concatenate(
                [p[t, :, 0:32].reshape(512, 128), p[t, :, 32:64].reshape(512, 128)], axis=1
            )
            block = got[2 * t + c, 0:SEQ].astype(F32) + dot(mixed[...], w)
            first[2 * t + c] = block
            total = total + jnp.sum(block, axis=1, keepdims=True)
    mean = total / 2048
    total = jnp.zeros((SEQ, 1), F32)
    for t in range(8):
        off = first[t] - mean
        total = total + jnp.sum(off * off, axis=1, keepdims=True)
    scale = lax.rsqrt(total / 2048 + EPS)
    for t in range(8):
        hmid[t] = ((first[t] - mean) * scale * gain_of(got, t, 1)).astype(BF)
    for i in range(2):
        keep[i] = first[2 * y + i]


def summed(src, acc, left, halves):
    for lo, hi in CHUNKS:
        right = jnp.concatenate([w[i, lo:hi] for w in halves for i in range(2)], axis=1)
        got = dot_t(left, right)
        acc[:, lo:hi] = got if src is None else src[:, lo:hi] + got


def add_a(src, acc, rows, zz, halves):
    left = jnp.concatenate([rows[2 * zz + p] for p, _ in halves], axis=1)
    summed(src, acc, left, [w for _, w in halves])


def add_b(src, acc, rows, xx, halves):
    lane = pl.ds(pl.multiple_of((xx % 2) * 128, 128), 128)
    left = jnp.concatenate(
        [rows[2 * (2 * p + i) + xx // 2, :, lane] for p, _ in halves for i in range(2)], axis=1
    )
    summed(src, acc, left, [w for _, w in halves])


def near(at, h0, h1, *refs):
    a0, a1, a3, b0, b1, b3 = [refs[2 * i : 2 * i + 2] for i in range(6)]
    acc_a, acc_b, rows = refs[12:]
    x, z = at[0], at[2]
    for t in range(8):
        rows[t, 0:SEQ] = h0[t]
        rows[t, SEQ:] = h1[t]
    for k, a in ((0, a0), (1, a1), (3, a3)):
        add_a(None if k == 0 else acc_a, acc_a, rows, (z + k) % 4, list(enumerate(a)))
    for k, b in ((0, b0), (1, b1), (3, b3)):
        add_b(None if k == 0 else acc_b, acc_b, rows, (x + k) % 4, list(enumerate(b)))


def far(at, rows, in_a, in_b, *refs):
    a_all = [refs[2 * i : 2 * i + 2] for i in range(4)]
    b_all = [refs[2 * i : 2 * i + 2] for i in range(4, 8)]
    mine, other, acc_a, acc_b, down, hidden = refs[16:]
    x, z = at[0], at[2]
    add_a(in_a, acc_a, rows, (z + 2) % 4, list(enumerate(a_all[2])))
    add_b(in_b, acc_b, rows, (x + 2) % 4, list(enumerate(b_all[2])))
    for k in range(4):
        for p in range(2):
            for i in range(2):
                down[(z + k) % 4 * 4 + 2 * p + i, 0:DA] = a_all[k][p][i, FF:]
                down[(2 * p + i) * 4 + (x + k) % 4, DA:] = b_all[k][p][i, FF:]
    for lo, hi in CHUNKS:
        hidden[:, lo:hi] = (silu(acc_a[:, lo:hi]) * acc_b[:, lo:hi]).astype(BF)
    for t in range(8):
        right = jnp.concatenate([down[2 * t], down[2 * t + 1]], axis=1)
        res = dot(hidden[...], right).astype(BF)
        mine[t] = res[0:SEQ]
        other[t] = res[SEQ:]


def chip_sum(at, mine, got, *outs):
    for k in range(4):
        t = (at[1] + 4 - k) % 4
        for i in range(2):
            outs[k][i] = (mine[2 * t + i].astype(F32) + got[2 * t + i].astype(F32)).astype(BF)


def residual(at, keep, p0, p1, p2, p3, second, stats):
    lane = lax.broadcasted_iota(jnp.int32, (SEQ, 128), 1)
    s0 = jnp.zeros((SEQ, 1), F32)
    s1 = jnp.zeros((SEQ, 1), F32)
    for i in range(2):
        v = keep[i]
        for p in (p0, p1, p2, p3):
            v = v + p[i].astype(F32)
        second[i] = v
        s0 = s0 + jnp.sum(v, axis=1, keepdims=True)
        s1 = s1 + jnp.sum(v * v, axis=1, keepdims=True)
    stats[...] = jnp.where(lane == 0, s0, jnp.where(lane == 1, s1, 0.0)).T[0:8]


def finish(at, got, second, s0, s1, s2, s3, keep, give):
    y, core = at[1], at[3]
    total = s0[...] + s1[...] + s2[...] + s3[...]
    cols = jnp.concatenate([total, jnp.zeros((120, SEQ), F32)], axis=0).T
    mean = cols[:, 0:1] / 2048
    var = cols[:, 1:2] / 2048 - mean * mean
    scale = lax.rsqrt(var + EPS)
    for out, c in ((keep, core), (give, 1 - core)):
        out[...] = ((second[c] - mean) * scale * gain_of(got, 2 * y + c, 3)).astype(BF)


def assemble(at, mine, other, out):
    core = at[3]
    for c, v in ((core, mine), (1 - core, other)):
        out[pl.ds(pl.multiple_of(c * SEQ, SEQ), SEQ)] = v[...]


def per_device(
    tokens,
    norm_gain,
    value_weight,
    glu_weight,
    conv_kernel,
    conv_gain,
    proj_weight,
    mlp_gain,
    gate_weight,
    up_weight,
    down_weight,
    out_gain,
):
    at = jnp.stack([lax.axis_index(n) for n in ("x", "y", "z", "core")]).astype(jnp.int32)

    (sent,) = call(
        pack_tokens,
        [((8, SEQ + EXTRA, 256), BF)],
        (at, tokens, norm_gain[None], mlp_gain[None], conv_gain[None], out_gain[None]),
    )
    got = exchange(sent, TP)

    (small,) = call(pack_small, [((192, 128), BF)], (at, value_weight.T, glu_weight.T, proj_weight))
    row_near = [x_from(small, k) for k in (1, 2, -1)]
    (row,) = call(pack_row, [((4, 192, 128), BF)], (at, small, *row_near))

    a, b = call(
        pack_weights,
        [((A_ROWS, 128), BF), ((B_ROWS, 128), BF)],
        (at, gate_weight.T, up_weight.T, down_weight),
    )
    half_a, half_b = ((2, A_ROWS, 128), BF), ((2, B_ROWS, 128), BF)
    b_near = [z_from(b, k) for k in (1, 2, -1)]
    a_near = [x_from(a, k) for k in (1, 2, -1)]
    b0 = call(pack_halves(2), [half_b] * 2, (at, b, *b_near))
    a0 = call(pack_halves(0), [half_a] * 2, (at, a, *a_near))
    b1 = [x_from(b0[0], 1), x_from(b0[1], 1)]
    b3 = [x_from(b0[0], -1), x_from(b0[1], -1)]
    a1 = [z_from(a0[0], 1), z_from(a0[1], 1)]
    a3 = [z_from(a0[0], -1), z_from(a0[1], -1)]
    b2 = [x_from(b1[0], 1), x_from(b3[1], -1)]
    a2 = [z_from(a1[0], 1), z_from(a3[1], -1)]

    vg, proj = call(
        pack_plane,
        [((16, 128, 128), BF), ((4, 16, 64, 128), BF)],
        (at, row, z_from(row, 1), z_from(row, 2), z_from(row, -1)),
    )
    vg_other = swap(vg)
    taps_other = swap(conv_kernel)
    proj = exchange(proj, "y")
    proj_other = swap(proj)

    (conv,) = call(
        module_in,
        [((SEQ, 128), BF)],
        (at, got, vg, vg_other, conv_kernel, taps_other),
        scratch=[((SEQ + 32, 128), F32)],
        flops=2 * SEQ * 2048 * 256,
    )
    hmid, keep = call(
        module_out,
        [((8, SEQ, 256), BF), ((2, SEQ, 256), F32)],
        (at, got, conv, y_from(conv, 1), y_from(conv, 2), y_from(conv, -1), proj, proj_other),
        scratch=[((8, SEQ, 256), F32), ((SEQ, 512), BF)],
        flops=2 * SEQ * 512 * 2048,
    )
    hmid_other = swap(hmid)

    acc_a, acc_b, rows = call(
        near,
        [((2 * SEQ, FF), F32), ((2 * SEQ, FF), F32), ((8, 2 * SEQ, 256), BF)],
        (at, hmid, hmid_other, *a0, *a1, *a3, *b0, *b1, *b3),
        flops=2 * 512 * 1536 * 1408,
    )
    mine, other = call(
        far,
        [((8, SEQ, 256), BF), ((8, SEQ, 256), BF)],
        (at, rows, acc_a, acc_b, *a0, *a1, *a2, *a3, *b0, *b1, *b2, *b3),
        scratch=[
            ((2 * SEQ, FF), F32),
            ((2 * SEQ, FF), F32),
            ((16, DA + DB, 128), BF),
            ((2 * SEQ, FF), BF),
        ],
        flops=2 * 512 * (512 * 1408 + 704 * 2048),
    )
    parts = call(chip_sum, [((2, SEQ, 256), BF)] * 4, (at, mine, swap(other)))
    second, stats = call(
        residual,
        [((2, SEQ, 256), F32), ((8, SEQ), F32)],
        (at, keep, parts[0], *(y_from(parts[k], k) for k in (1, 2, 3))),
    )
    kept, given = call(
        finish,
        [((SEQ, 256), BF), ((SEQ, 256), BF)],
        (at, got, second, stats, *(y_from(stats, k) for k in (1, 2, 3))),
    )
    (out,) = call(assemble, [((2 * SEQ, 256), BF)], (at, kept, swap(given)))
    return out


def solution(mesh):
    split = Mesh(mesh.devices.reshape(2, 4, 4, 4, 2), ("rep", "z", "x", "y", "core"))
    rows, fs, tp = ("rep", "z", "x"), ("z", "x"), ("y", "core")
    in_specs = (
        P(rows, tp),
        P(tp),
        P(fs, tp),
        P(fs, tp),
        P(None, tp),
        P(tp),
        P(fs, tp),
        P(tp),
        P(fs, tp),
        P(fs, tp),
        P(tp, fs),
        P(tp),
    )
    return jax.shard_map(
        per_device, mesh=split, in_specs=in_specs, out_specs=P(rows, tp), check_vma=False
    )
```

```python
import functools

import jax
import jax.numpy as jnp
from jax import lax
from jax.experimental import pallas as pl
from jax.experimental.pallas import tpu as pltpu
from jax.sharding import Mesh
from jax.sharding import PartitionSpec as P


EPS = 1e-05
Z = ("rep", "z")
TP = ("y", "core")
BF = jnp.bfloat16
F32 = jnp.float32
SEQ = 256
TAPS = 31
FF, SMALL = 704, 192
A_ROWS, B_ROWS = FF, 2 * FF
CHUNKS = ((0, 256), (256, 512), (512, 704))
EXTRA = 16


def call(body, outs, args, scratch=(), flops=0, hbm=(), copies=0, limit=None, out_space=pltpu.VMEM):
    size = sum(a.size * a.dtype.itemsize for a in args) + sum(
        functools.reduce(lambda p, q: p * q, s, 1) * jnp.dtype(d).itemsize for s, d in outs
    )
    held = sum(
        functools.reduce(lambda p, q: p * q, s, 1) * jnp.dtype(d).itemsize for s, d in scratch
    )
    return pl.pallas_call(
        body,
        out_shape=[jax.ShapeDtypeStruct(s, d) for s, d in outs],
        in_specs=[pl.BlockSpec(memory_space=pltpu.SMEM)]
        + [pl.BlockSpec(memory_space=pltpu.VMEM)] * (len(args) - 1)
        + [pl.BlockSpec(memory_space=pltpu.HBM)] * len(hbm),
        out_specs=[pl.BlockSpec(memory_space=out_space)] * len(outs),
        scratch_shapes=[pltpu.VMEM(s, d) for s, d in scratch]
        + ([pltpu.SemaphoreType.DMA((copies,))] if copies else []),
        compiler_params=pltpu.CompilerParams(vmem_limit_bytes=limit or size + held + (6 << 20)),
        cost_estimate=pl.CostEstimate(
            flops=max(flops, size * 300), bytes_accessed=size, transcendentals=0
        ),
    )(*args, *hbm)


def ring(x, axes, step, size):
    return lax.ppermute(x, axes, [((i + step) % size, i) for i in range(size)])


def y_from(x, step):
    return ring(x, "y", step, 4)


def x_from(x, step):
    return ring(x, "x", step, 4)


def z_from(x, step):
    if step == 2:
        return lax.ppermute(x, Z, [((i + (2 if i % 2 == 0 else -2)) % 8, i) for i in range(8)])
    return ring(x, Z, step, 8)


def swap(x):
    return lax.ppermute(x, "core", [(0, 1), (1, 0)])


def exchange(x, axes):
    return lax.all_to_all(x, axes, 0, 0, tiled=True)


class Copies:
    def __init__(self, sems):
        self.sems, self.count = sems, 0

    def start(self, src, dst):
        copy = pltpu.make_async_copy(src, dst, self.sems.at[self.count])
        self.count += 1
        copy.start()
        return copy


def dot(a, b):
    return jnp.dot(a, b, preferred_element_type=F32)


def dot_t(a, b):
    return lax.dot_general(a, b, (((1,), (1,)), ((), ())), preferred_element_type=F32)


def silu(v):
    return v * jax.nn.sigmoid(v)


def pack_all(at, tokens, g0, g1, g2, g3, gate, up, down, value, glu, proj, sent, a, b, *refs):
    norm_gain, mlp_gain, conv_gain, out_gain, rows, packed_a, packed_b, params, sems = refs
    copies = Copies(sems)
    into_b = [
        copies.start(up, packed_b.at[pl.ds(0, FF)]),
        copies.start(down, packed_b.at[pl.ds(FF, FF)]),
    ]
    into_a = [
        copies.start(src, packed_a.at[pl.ds(first, count)])
        for src, first, count in (
            (gate, 0, FF),
            (value, A_ROWS, 64),
            (glu, A_ROWS + 64, 64),
            (proj.at[:, pl.ds(0, 128)], A_ROWS + 128, 32),
            (proj.at[:, pl.ds(128, 128)], A_ROWS + 160, 32),
        )
    ]
    pairs = ((g0, norm_gain), (g1, mlp_gain), (g2, conv_gain), (g3, out_gain))
    gains = [copies.start(src, dst) for src, dst in pairs]
    into_rows = copies.start(tokens, rows)
    for copy in into_b:
        copy.wait()
    out = [copies.start(packed_b, b)]
    for copy in into_a:
        copy.wait()
    out.append(copies.start(packed_a, a))
    into_rows.wait()
    for t in range(8):
        out.append(copies.start(rows.at[pl.ds(t % 2 * SEQ, SEQ)], sent.at[t, pl.ds(0, SEQ)]))
    for copy in gains:
        copy.wait()
    row = lax.broadcasted_iota(jnp.int32, (EXTRA, 256), 0)
    extra = jnp.zeros((EXTRA, 256), F32)
    wide = jnp.concatenate([conv_gain[...], jnp.zeros((1, 192), F32)], axis=1)
    for i, g in enumerate((norm_gain[...], mlp_gain[...], wide, out_gain[...])):
        high = g.astype(BF).astype(F32)
        mid = (g - high).astype(BF).astype(F32)
        low = g - high - mid
        for j, part in enumerate((high, mid, low)):
            extra = jnp.where(row == 3 * i + j, part, extra)
    params[...] = extra.astype(BF)
    for t in range(8):
        out.append(copies.start(params, sent.at[t, pl.ds(SEQ, EXTRA)]))
    for copy in out:
        copy.wait()


def gain_of(got, t, i):
    rows = got[t, SEQ:].astype(F32)
    return rows[3 * i : 3 * i + 1] + rows[3 * i + 1 : 3 * i + 2] + rows[3 * i + 2 : 3 * i + 3]


def pack_a(at, p0, p1, p2, p3, out, small):
    for k, p in enumerate((p0, p1, p2, p3)):
        i = (at[0] + k) % 4
        out[i] = p[0:A_ROWS]
        small[i] = p[A_ROWS:]


def pack_b(at, p0, p1, p2, p3, low, high):
    for k, p in enumerate((p0, p1, p2, p3)):
        i = (at[2] + k) % 4

        @pl.when(i < 2)
        def _():
            low[i] = p[...]

        @pl.when(i >= 2)
        def _():
            high[i - 2] = p[...]


def pack_plane(at, s0, s1, s2, s3, vg, proj):
    for k, s in enumerate((s0, s1, s2, s3)):
        zz = (at[2] + k) % 4
        for i in range(4):
            vg[zz * 4 + i] = s[i, 0:128]
            proj[zz * 4 + i] = s[i, 128:192]


def module_in(at, got, vg, vg_other, taps, taps_other, out, padded):
    core = at[3]
    total = jnp.zeros((SEQ, 1), F32)
    for t in range(8):
        total = total + jnp.sum(got[t, 0:SEQ].astype(F32), axis=1, keepdims=True)
    mean = total / 2048
    total = jnp.zeros((SEQ, 1), F32)
    for t in range(8):
        off = got[t, 0:SEQ].astype(F32) - mean
        total = total + jnp.sum(off * off, axis=1, keepdims=True)
    scale = lax.rsqrt(total / 2048 + EPS)

    def step(t, acc):
        hin = ((got[t, 0:SEQ].astype(F32) - mean) * scale * gain_of(got, t, 0)).astype(BF)
        w = jnp.concatenate(
            [jnp.concatenate([v[2 * t], v[2 * t + 1]], axis=1) for v in (vg, vg_other)], axis=0
        )
        return acc + dot_t(hin, w)

    acc = lax.fori_loop(0, 8, step, jnp.zeros((SEQ, 256), F32), unroll=4)
    both = acc.astype(BF).astype(F32)
    lane = lax.broadcasted_iota(jnp.int32, (SEQ, 128), 1)

    def gated(v):
        return v * jax.nn.sigmoid(pltpu.roll(v, 64, 1))

    mine, other = gated(both[:, 0:128]), gated(both[:, 128:256])
    is0 = core == 0
    unit = jnp.where(
        lane < 64,
        jnp.where(is0, mine, other),
        pltpu.roll(jnp.where(is0, other, mine), 64, 1),
    )
    padded[0:32] = jnp.zeros((32, 128), F32)
    padded[32:] = unit
    ta, tb = taps[...].astype(F32), taps_other[...].astype(F32)
    first, second = jnp.where(is0, ta, tb), jnp.where(is0, tb, ta)
    k = jnp.concatenate([first, second], axis=1)
    conv = jnp.zeros((SEQ, 128), F32)
    for s in range(TAPS):
        conv = conv + k[s : s + 1] * padded[32 - s : 32 - s + SEQ]
    out[...] = conv.astype(BF)


def module_out(at, got, c0, c1, c2, c3, *refs):
    y, core = at[1], at[3]
    conv = (c0, c1, c2, c3)
    hmid, keep, first, mixed = refs[8:]
    total = jnp.zeros((SEQ, 1), F32)
    for k in range(4):
        total = total + jnp.sum(conv[k][...].astype(F32), axis=1, keepdims=True)
    mean = total / 512
    total = jnp.zeros((SEQ, 1), F32)
    for k in range(4):
        off = conv[k][...].astype(F32) - mean
        total = total + jnp.sum(off * off, axis=1, keepdims=True)
    scale = lax.rsqrt(total / 512 + EPS)
    for k in range(4):
        t = (y + k) % 4
        gain = jnp.concatenate(
            [gain_of(got, 2 * t, 2)[:, 0:64], gain_of(got, 2 * t + 1, 2)[:, 0:64]], axis=1
        )
        mixed[:, pl.ds(pl.multiple_of(t * 128, 128), 128)] = silu(
            (conv[k][...].astype(F32) - mean) * scale * gain
        ).astype(BF)

    total = jnp.zeros((SEQ, 1), F32)
    for k in range(4):
        t = (y + k) % 4
        for p, c in ((refs[k], core), (refs[4 + k], 1 - core)):
            w = jnp.concatenate(
                [p[:, 0:32].reshape(512, 128), p[:, 32:64].reshape(512, 128)], axis=1
            )
            block = got[2 * t + c, 0:SEQ].astype(F32) + dot(mixed[...], w)
            first[2 * t + c] = block
            total = total + jnp.sum(block, axis=1, keepdims=True)
    mean = total / 2048
    total = jnp.zeros((SEQ, 1), F32)
    for t in range(8):
        off = first[t] - mean
        total = total + jnp.sum(off * off, axis=1, keepdims=True)
    scale = lax.rsqrt(total / 2048 + EPS)
    for t in range(8):
        hmid[t] = ((first[t] - mean) * scale * gain_of(got, t, 1)).astype(BF)
    for i in range(2):
        keep[i] = first[2 * y + i]


def lay_out(h0, h1, ha, hb, steps, x, z):
    for row, h in ((0, h0), (SEQ, h1)):
        for n, k in enumerate(steps):
            zz, xx = (z + k) % 4, (x + k) % 4
            lane = pl.ds(pl.multiple_of((xx % 2) * 128, 128), 128)
            for p in range(2):
                c = (4 * n + 2 * p) * 128
                ha[row : row + SEQ, c : c + 256] = h[2 * zz + p]
            for i in range(4):
                c = (4 * n + i) * 128
                hb[row : row + SEQ, c : c + 128] = h[2 * i + xx // 2, :, lane]


def gate_up(copies, a_pieces, b_pieces, wa, wb):
    into_a = [
        copies.start(p.at[i], wa.at[:, pl.ds((4 * n + i) * 128, 128)])
        for n, p in enumerate(a_pieces)
        for i in range(4)
    ]
    into_b = [
        copies.start(p.at[i, pl.ds(0, FF)], wb.at[:, pl.ds((2 * n + i) * 128, 128)])
        for n, p in enumerate(b_pieces)
        for i in range(2)
    ]
    return into_a, into_b


def near(at, h0, h1, a0, a1, a3, *refs):
    acc_a, acc_b, wa, wb, ha, hb, sems = refs[6:]
    started = gate_up(Copies(sems), (a0, a1, a3), refs[:6], wa, wb)
    lay_out(h0, h1, ha, hb, (0, 1, 3), at[0], at[2])
    for into, acc, h, w in zip(started, (acc_a, acc_b), (ha, hb), (wa, wb)):
        for copy in into:
            copy.wait()
        for lo, hi in CHUNKS:
            acc[:, lo:hi] = dot_t(h[...], w[lo:hi])


def far(at, h0, h1, in_a, in_b, a2, *refs):
    mine, other, wa, wb, down, ha, hb, hidden, sems = refs[8:]
    x, z = at[0], at[2]
    copies = Copies(sems)
    into_a, into_b = gate_up(copies, (a2,), refs[4:6], wa, wb)
    into_down = [
        copies.start(
            refs[2 * k + p].at[i, pl.ds(FF, FF)], down.at[(2 * p + i) * 4 + (x + k) % 4]
        )
        for k in range(4)
        for p in range(2)
        for i in range(2)
    ]
    lay_out(h0, h1, ha, hb, (2,), x, z)
    for copy in into_a + into_b:
        copy.wait()
    for lo, hi in CHUNKS:
        gates = in_a[:, lo:hi] + dot_t(ha[...], wa[lo:hi])
        ups = in_b[:, lo:hi] + dot_t(hb[...], wb[lo:hi])
        hidden[:, lo:hi] = (silu(gates) * ups).astype(BF)
    for copy in into_down:
        copy.wait()

    @pl.loop(0, 8, unroll=2)
    def _(t):
        right = jnp.concatenate([down[2 * t], down[2 * t + 1]], axis=1)
        res = dot(hidden[...], right).astype(BF)
        mine[t] = res[0:SEQ]
        other[t] = res[SEQ:]


def chip_sum(at, mine, got, *outs):
    for k in range(4):
        t = (at[1] + 4 - k) % 4
        for i in range(2):
            outs[k][i] = (mine[2 * t + i].astype(F32) + got[2 * t + i].astype(F32)).astype(BF)


def residual(at, keep, p0, p1, p2, p3, second, stats):
    lane = lax.broadcasted_iota(jnp.int32, (SEQ, 128), 1)
    s0 = jnp.zeros((SEQ, 1), F32)
    s1 = jnp.zeros((SEQ, 1), F32)
    for i in range(2):
        v = keep[i]
        for p in (p0, p1, p2, p3):
            v = v + p[i].astype(F32)
        second[i] = v
        s0 = s0 + jnp.sum(v, axis=1, keepdims=True)
        s1 = s1 + jnp.sum(v * v, axis=1, keepdims=True)
    stats[...] = jnp.where(lane == 0, s0, jnp.where(lane == 1, s1, 0.0)).T[0:8]


def finish(at, got, second, s0, s1, s2, s3, keep, give):
    y, core = at[1], at[3]
    total = s0[...] + s1[...] + s2[...] + s3[...]
    cols = jnp.concatenate([total, jnp.zeros((120, SEQ), F32)], axis=0).T
    mean = cols[:, 0:1] / 2048
    var = cols[:, 1:2] / 2048 - mean * mean
    scale = lax.rsqrt(var + EPS)
    for out, c in ((keep, core), (give, 1 - core)):
        out[...] = ((second[c] - mean) * scale * gain_of(got, 2 * y + c, 3)).astype(BF)


def assemble(at, mine, other, out):
    core = at[3]
    for c, v in ((core, mine), (1 - core, other)):
        out[pl.ds(pl.multiple_of(c * SEQ, SEQ), SEQ)] = v[...]


def per_device(
    tokens,
    norm_gain,
    value_weight,
    glu_weight,
    conv_kernel,
    conv_gain,
    proj_weight,
    mlp_gain,
    gate_weight,
    up_weight,
    down_weight,
    out_gain,
):
    at = jnp.stack([lax.axis_index(n) for n in ("x", "y", "z", "core")]).astype(jnp.int32)

    sent, a, b = call(
        pack_all,
        [((8, SEQ + EXTRA, 256), BF), ((A_ROWS + SMALL, 128), BF), ((B_ROWS, 128), BF)],
        (at,),
        hbm=(
            tokens,
            norm_gain[None],
            mlp_gain[None],
            conv_gain[None],
            out_gain[None],
            gate_weight.T,
            up_weight.T,
            down_weight,
            value_weight.T,
            glu_weight.T,
            proj_weight,
        ),
        scratch=[
            ((1, 256), F32),
            ((1, 256), F32),
            ((1, 64), F32),
            ((1, 256), F32),
            ((2 * SEQ, 256), BF),
            ((A_ROWS + SMALL, 128), BF),
            ((B_ROWS, 128), BF),
            ((EXTRA, 256), BF),
        ],
        copies=30,
        limit=67043328,
        out_space=pltpu.HBM,
    )
    got = exchange(sent, TP)

    b_near = [z_from(b, k) for k in (1, 2, -1)]
    a_near = [x_from(a, k) for k in (1, 2, -1)]
    a0, row = call(pack_a, [((4, A_ROWS, 128), BF), ((4, SMALL, 128), BF)], (at, a, *a_near))
    b0 = call(pack_b, [((2, B_ROWS, 128), BF)] * 2, (at, b, *b_near))
    a1, a2, a3 = z_from(a0, 1), z_from(a0, 2), z_from(a0, -1)
    b1 = [x_from(b0[0], 1), x_from(b0[1], 1)]
    b3 = [x_from(b0[0], -1), x_from(b0[1], -1)]
    b2 = [x_from(b1[0], 1), x_from(b3[1], -1)]

    vg, proj = call(
        pack_plane,
        [((16, 128, 128), BF), ((16, 64, 128), BF)],
        (at, row, z_from(row, 1), z_from(row, 2), z_from(row, -1)),
    )
    vg_other = swap(vg)
    taps_other = swap(conv_kernel)
    projs = [proj] + [y_from(proj, k) for k in (1, 2, 3)]
    projs += [swap(p) for p in projs]

    (conv,) = call(
        module_in,
        [((SEQ, 128), BF)],
        (at, got, vg, vg_other, conv_kernel, taps_other),
        scratch=[((SEQ + 32, 128), F32)],
        flops=2 * SEQ * 2048 * 256,
    )
    hmid, keep = call(
        module_out,
        [((8, SEQ, 256), BF), ((2, SEQ, 256), F32)],
        (at, got, conv, y_from(conv, 1), y_from(conv, 2), y_from(conv, -1), *projs),
        scratch=[((8, SEQ, 256), F32), ((SEQ, 512), BF)],
        flops=2 * SEQ * 512 * 2048,
    )
    hmid_other = swap(hmid)

    acc_a, acc_b = call(
        near,
        [((2 * SEQ, FF), F32), ((2 * SEQ, FF), F32)],
        (at, hmid, hmid_other),
        hbm=(a0, a1, a3, *b0, *b1, *b3),
        scratch=[
            ((FF, 1536), BF),
            ((FF, 1536), BF),
            ((2 * SEQ, 1536), BF),
            ((2 * SEQ, 1536), BF),
        ],
        flops=2 * 512 * 1536 * 1408,
        copies=24,
    )
    mine, other = call(
        far,
        [((8, SEQ, 256), BF), ((8, SEQ, 256), BF)],
        (at, hmid, hmid_other, acc_a, acc_b),
        hbm=(a2, *b0, *b1, *b2, *b3),
        scratch=[
            ((FF, 512), BF),
            ((FF, 512), BF),
            ((16, FF, 128), BF),
            ((2 * SEQ, 512), BF),
            ((2 * SEQ, 512), BF),
            ((2 * SEQ, FF), BF),
        ],
        flops=2 * 512 * 704 * (2048 + 1024),
        copies=24,
    )
    parts = call(chip_sum, [((2, SEQ, 256), BF)] * 4, (at, mine, swap(other)))
    second, stats = call(
        residual,
        [((2, SEQ, 256), F32), ((8, SEQ), F32)],
        (at, keep, parts[0], *(y_from(parts[k], k) for k in (1, 2, 3))),
    )
    kept, given = call(
        finish,
        [((SEQ, 256), BF), ((SEQ, 256), BF)],
        (at, got, second, stats, *(y_from(stats, k) for k in (1, 2, 3))),
    )
    (out,) = call(assemble, [((2 * SEQ, 256), BF)], (at, kept, swap(given)))
    return out


def solution(mesh):
    split = Mesh(mesh.devices.reshape(2, 4, 4, 4, 2), ("rep", "z", "x", "y", "core"))
    rows, fs, tp = ("rep", "z", "x"), ("z", "x"), ("y", "core")
    in_specs = (
        P(rows, tp),
        P(tp),
        P(fs, tp),
        P(fs, tp),
        P(None, tp),
        P(tp),
        P(fs, tp),
        P(tp),
        P(fs, tp),
        P(fs, tp),
        P(tp, fs),
        P(tp),
    )
    return jax.shard_map(
        per_device, mesh=split, in_specs=in_specs, out_specs=P(rows, tp), check_vma=False
    )
```

```python
import functools

import jax
import jax.numpy as jnp
from jax import lax
from jax.experimental import pallas as pl
from jax.experimental.pallas import tpu as pltpu
from jax.sharding import Mesh
from jax.sharding import PartitionSpec as P


EPS = 1e-05
Z = ("rep", "z")
TP = ("y", "core")
BF = jnp.bfloat16
F32 = jnp.float32
SEQ = 256
TAPS = 31
FF, SMALL = 704, 192
A_ROWS, B_ROWS = FF, 2 * FF
EXTRA = 16


def call(body, outs, args, scratch=(), flops=0, hbm=(), copies=0, limit=None, out_space=pltpu.VMEM, alias=None):
    size = sum(a.size * a.dtype.itemsize for a in args) + sum(
        functools.reduce(lambda p, q: p * q, s, 1) * jnp.dtype(d).itemsize for s, d in outs
    )
    held = sum(
        functools.reduce(lambda p, q: p * q, s, 1) * jnp.dtype(d).itemsize for s, d in scratch
    )
    return pl.pallas_call(
        body,
        out_shape=[jax.ShapeDtypeStruct(s, d) for s, d in outs],
        in_specs=[pl.BlockSpec(memory_space=pltpu.SMEM)]
        + [pl.BlockSpec(memory_space=pltpu.VMEM)] * (len(args) - 1)
        + [pl.BlockSpec(memory_space=pltpu.HBM)] * len(hbm),
        out_specs=[pl.BlockSpec(memory_space=out_space)] * len(outs),
        scratch_shapes=[pltpu.VMEM(s, d) for s, d in scratch]
        + ([pltpu.SemaphoreType.DMA((copies,))] if copies else []),
        compiler_params=pltpu.CompilerParams(vmem_limit_bytes=limit or size + held + (6 << 20)),
        cost_estimate=pl.CostEstimate(
            flops=max(flops, size * 10), bytes_accessed=size, transcendentals=0
        ),
        input_output_aliases=alias or {},
    )(*args, *hbm)


def ring(x, axes, step, size):
    return lax.ppermute(x, axes, [((i + step) % size, i) for i in range(size)])


def y_from(x, step):
    return ring(x, "y", step, 4)


def x_from(x, step):
    return ring(x, "x", step, 4)


def z_from(x, step):
    if step == 2:
        return lax.ppermute(x, Z, [((i + (2 if i % 2 == 0 else -2)) % 8, i) for i in range(8)])
    return ring(x, Z, step, 8)


def swap(x):
    return lax.ppermute(x, "core", [(0, 1), (1, 0)])


def exchange(x, axes):
    return lax.all_to_all(x, axes, 0, 0, tiled=True)


class Copies:
    def __init__(self, sems):
        self.sems, self.count = sems, 0

    def start(self, src, dst):
        copy = pltpu.make_async_copy(src, dst, self.sems.at[self.count])
        self.count += 1
        copy.start()
        return copy


def dot(a, b):
    return jnp.dot(a, b, preferred_element_type=F32)


def dot_t(a, b):
    return lax.dot_general(a, b, (((1,), (1,)), ((), ())), preferred_element_type=F32)


def for_units(body):
    @pl.loop(0, 2)
    def _(j):
        body(pl.ds(pl.multiple_of(j * 256, 256), 256))

    body(pl.ds(512, FF - 512))


def silu(v):
    return v * jax.nn.sigmoid(v)


def pack_all(at, tokens, g0, g1, g2, g3, gate, up, down, value, glu, proj, sent, a, b, *refs):
    norm_gain, mlp_gain, conv_gain, out_gain, rows, packed_a, packed_b, params, sems = refs
    copies = Copies(sems)
    into_b = [
        copies.start(up, packed_b.at[pl.ds(0, FF)]),
        copies.start(down, packed_b.at[pl.ds(FF, FF)]),
    ]
    into_a = [
        copies.start(src, packed_a.at[pl.ds(first, count)])
        for src, first, count in (
            (gate, 0, FF),
            (value, A_ROWS, 64),
            (glu, A_ROWS + 64, 64),
            (proj.at[:, pl.ds(0, 128)], A_ROWS + 128, 32),
            (proj.at[:, pl.ds(128, 128)], A_ROWS + 160, 32),
        )
    ]
    pairs = ((g0, norm_gain), (g1, mlp_gain), (g2, conv_gain), (g3, out_gain))
    gains = [copies.start(src, dst) for src, dst in pairs]
    into_rows = copies.start(tokens, rows)
    for copy in into_b:
        copy.wait()
    out = [copies.start(packed_b, b)]
    for copy in into_a:
        copy.wait()
    out.append(copies.start(packed_a, a))
    into_rows.wait()
    for t in range(8):
        out.append(copies.start(rows.at[pl.ds(t % 2 * SEQ, SEQ)], sent.at[t, pl.ds(0, SEQ)]))
    for copy in gains:
        copy.wait()
    row = lax.broadcasted_iota(jnp.int32, (EXTRA, 256), 0)
    extra = jnp.zeros((EXTRA, 256), F32)
    wide = jnp.concatenate([conv_gain[...], jnp.zeros((1, 192), F32)], axis=1)
    for i, g in enumerate((norm_gain[...], mlp_gain[...], wide, out_gain[...])):
        high = g.astype(BF).astype(F32)
        mid = (g - high).astype(BF).astype(F32)
        low = g - high - mid
        for j, part in enumerate((high, mid, low)):
            extra = jnp.where(row == 3 * i + j, part, extra)
    params[...] = extra.astype(BF)
    for t in range(8):
        out.append(copies.start(params, sent.at[t, pl.ds(SEQ, EXTRA)]))
    for copy in out:
        copy.wait()


def gain_of(got, t, i):
    rows = got[t, SEQ:].astype(F32)
    return rows[3 * i : 3 * i + 1] + rows[3 * i + 1 : 3 * i + 2] + rows[3 * i + 2 : 3 * i + 3]


def pack_a(at, p0, p1, p2, p3, out, small):
    for k, p in enumerate((p0, p1, p2, p3)):
        i = (at[0] + k) % 4
        out[i] = p[0:A_ROWS]
        small[i] = p[A_ROWS:]


def pack_b(at, p0, p1, p2, p3, low, high):
    for k, p in enumerate((p0, p1, p2, p3)):
        i = (at[2] + k) % 4

        @pl.when(i < 2)
        def _():
            low[i] = p[...]

        @pl.when(i >= 2)
        def _():
            high[i - 2] = p[...]


def pack_plane(at, s0, s1, s2, s3, vg, proj):
    for k, s in enumerate((s0, s1, s2, s3)):
        zz = (at[2] + k) % 4
        for i in range(4):
            vg[zz * 4 + i] = s[i, 0:128]
            proj[zz * 4 + i] = s[i, 128:192]


def module_in(at, got, vg, vg_other, taps, taps_other, out, padded):
    core = at[3]
    total = jnp.zeros((SEQ, 1), F32)
    for t in range(8):
        total = total + jnp.sum(got[t, 0:SEQ].astype(F32), axis=1, keepdims=True)
    mean = total / 2048
    total = jnp.zeros((SEQ, 1), F32)
    for t in range(8):
        off = got[t, 0:SEQ].astype(F32) - mean
        total = total + jnp.sum(off * off, axis=1, keepdims=True)
    scale = lax.rsqrt(total / 2048 + EPS)

    def step(t, acc):
        hin = ((got[t, 0:SEQ].astype(F32) - mean) * scale * gain_of(got, t, 0)).astype(BF)
        w = jnp.concatenate(
            [jnp.concatenate([v[2 * t], v[2 * t + 1]], axis=1) for v in (vg, vg_other)], axis=0
        )
        return acc + dot_t(hin, w)

    acc = lax.fori_loop(0, 8, step, jnp.zeros((SEQ, 256), F32), unroll=4)
    both = acc.astype(BF).astype(F32)
    lane = lax.broadcasted_iota(jnp.int32, (SEQ, 128), 1)

    def gated(v):
        return v * jax.nn.sigmoid(pltpu.roll(v, 64, 1))

    mine, other = gated(both[:, 0:128]), gated(both[:, 128:256])
    is0 = core == 0
    unit = jnp.where(
        lane < 64,
        jnp.where(is0, mine, other),
        pltpu.roll(jnp.where(is0, other, mine), 64, 1),
    )
    padded[0:32] = jnp.zeros((32, 128), F32)
    padded[32:] = unit
    ta, tb = taps[...].astype(F32), taps_other[...].astype(F32)
    first, second = jnp.where(is0, ta, tb), jnp.where(is0, tb, ta)
    k = jnp.concatenate([first, second], axis=1)
    conv = jnp.zeros((SEQ, 128), F32)
    for s in range(TAPS):
        conv = conv + k[s : s + 1] * padded[32 - s : 32 - s + SEQ]
    out[...] = conv.astype(BF)


def module_out(at, got, c0, c1, c2, c3, *refs):
    y, core = at[1], at[3]
    conv = (c0, c1, c2, c3)
    hmid, keep, first, mixed = refs[8:]
    total = jnp.zeros((SEQ, 1), F32)
    for k in range(4):
        total = total + jnp.sum(conv[k][...].astype(F32), axis=1, keepdims=True)
    mean = total / 512
    total = jnp.zeros((SEQ, 1), F32)
    for k in range(4):
        off = conv[k][...].astype(F32) - mean
        total = total + jnp.sum(off * off, axis=1, keepdims=True)
    scale = lax.rsqrt(total / 512 + EPS)
    for k in range(4):
        t = (y + k) % 4
        gain = jnp.concatenate(
            [gain_of(got, 2 * t, 2)[:, 0:64], gain_of(got, 2 * t + 1, 2)[:, 0:64]], axis=1
        )
        mixed[:, pl.ds(pl.multiple_of(t * 128, 128), 128)] = silu(
            (conv[k][...].astype(F32) - mean) * scale * gain
        ).astype(BF)

    total = jnp.zeros((SEQ, 1), F32)
    for k in range(4):
        t = (y + k) % 4
        for p, c in ((refs[k], core), (refs[4 + k], 1 - core)):
            w = jnp.concatenate(
                [p[:, 0:32].reshape(512, 128), p[:, 32:64].reshape(512, 128)], axis=1
            )
            block = got[2 * t + c, 0:SEQ].astype(F32) + dot(mixed[...], w)
            first[2 * t + c] = block
            total = total + jnp.sum(block, axis=1, keepdims=True)
    mean = total / 2048
    total = jnp.zeros((SEQ, 1), F32)
    for t in range(8):
        off = first[t] - mean
        total = total + jnp.sum(off * off, axis=1, keepdims=True)
    scale = lax.rsqrt(total / 2048 + EPS)
    for t in range(8):
        hmid[t] = ((first[t] - mean) * scale * gain_of(got, t, 1)).astype(BF)
    for i in range(2):
        keep[i] = first[2 * y + i]


def lay_a(h0, h1, ha, z):
    for row, h in ((0, h0), (SEQ, h1)):
        for n, k in enumerate((0, 1, 3, 2)):
            for p in range(2):
                c = (4 * n + 2 * p) * 128
                ha[row : row + SEQ, c : c + 256] = h[2 * ((z + k) % 4) + p]


def lay_b(h0, h1, hb, x, steps):
    for row, h in ((0, h0), (SEQ, h1)):
        for n, k in enumerate(steps):
            xx = (x + k) % 4
            lane = pl.ds(pl.multiple_of((xx % 2) * 128, 128), 128)
            for i in range(4):
                c = (4 * n + i) * 128
                hb[row : row + SEQ, c : c + 128] = h[2 * i + xx // 2, :, lane]


def fetch_b(copies, pieces, wb):
    return [
        copies.start(p.at[i, pl.ds(0, FF)], wb.at[:, pl.ds((2 * n + i) * 128, 128)])
        for n, p in enumerate(pieces)
        for i in range(2)
    ]


def fetch_down(copies, pieces, steps, x, down):
    return [
        copies.start(
            pieces[2 * n + p].at[i, pl.ds(FF, FF)], down.at[(2 * p + i) * 4 + (x + k) % 4]
        )
        for n, k in enumerate(steps)
        for p in range(2)
        for i in range(2)
    ]


def near(at, h0, h1, a0, a1, a3, a2, *refs):
    gates, acc_b, down, wa, wb, ha, hb, sems = refs[6:]
    x, z = at[0], at[2]
    copies = Copies(sems)
    into_b = fetch_b(copies, refs[:6], wb)
    into_a = [
        copies.start(p.at[i], wa.at[:, pl.ds((4 * n + i) * 128, 128)])
        for n, p in enumerate((a0, a1, a3, a2))
        for i in range(4)
    ]
    into_down = fetch_down(copies, refs[:6], (0, 1, 3), x, down)
    lay_b(h0, h1, hb, x, (0, 1, 3))
    lay_a(h0, h1, ha, z)
    for copy in into_b:
        copy.wait()

    @for_units
    def _(units):
        acc_b[:, units] = dot_t(hb[...], wb[units])

    for copy in into_a:
        copy.wait()

    @for_units
    def _(units):
        gates[:, units] = silu(dot_t(ha[...], wa[units]))

    for copy in into_down:
        copy.wait()


def products(hidden, down, mine, other, chip, stride):
    @pl.loop(0, 2)
    def _(j):
        for i in range(2):
            t = 2 * ((chip + stride * j) % 4) + i
            right = jnp.concatenate([down[2 * t], down[2 * t + 1]], axis=1)
            res = dot(hidden[...], right).astype(BF)
            mine[2 * j + i] = res[0:SEQ]
            other[2 * j + i] = res[SEQ:]


def far(at, h0, h1, gates, acc_b, down_in, b2l, b2h, mine, other, hidden, down, wb, hb, sems):
    x, y = at[0], at[1]
    copies = Copies(sems)
    into_b = fetch_b(copies, (b2l, b2h), wb)
    into_down = fetch_down(copies, (b2l, b2h), (2,), x, down)
    lay_b(h0, h1, hb, x, (2,))
    for copy in into_b:
        copy.wait()

    @for_units
    def _(units):
        ups = acc_b[:, units] + dot_t(hb[...], wb[units])
        hidden[:, units] = (gates[:, units] * ups).astype(BF)

    for copy in into_down:
        copy.wait()
    products(hidden, down, mine, other, y + 2, 1)


def rest(at, hidden, down, mine, other):
    products(hidden, down, mine, other, at[1] + 1, 3)


def chip_sum(at, mine, got, *outs):
    for j in range(2):
        for i in range(2):
            t = 2 * j + i
            outs[j][i] = (mine[t].astype(F32) + got[t].astype(F32)).astype(BF)


def residual(at, keep, p0, p1, p2, p3, second, stats):
    lane = lax.broadcasted_iota(jnp.int32, (SEQ, 128), 1)
    s0 = jnp.zeros((SEQ, 1), F32)
    s1 = jnp.zeros((SEQ, 1), F32)
    for i in range(2):
        v = keep[i]
        for p in (p0, p1, p2, p3):
            v = v + p[i].astype(F32)
        second[i] = v
        s0 = s0 + jnp.sum(v, axis=1, keepdims=True)
        s1 = s1 + jnp.sum(v * v, axis=1, keepdims=True)
    stats[...] = jnp.where(lane == 0, s0, jnp.where(lane == 1, s1, 0.0)).T[0:8]


def finish(at, got, second, s0, s1, s2, s3, keep, give):
    y, core = at[1], at[3]
    total = s0[...] + s1[...] + s2[...] + s3[...]
    cols = jnp.concatenate([total, jnp.zeros((120, SEQ), F32)], axis=0).T
    mean = cols[:, 0:1] / 2048
    var = cols[:, 1:2] / 2048 - mean * mean
    scale = lax.rsqrt(var + EPS)
    for out, c in ((keep, core), (give, 1 - core)):
        out[...] = ((second[c] - mean) * scale * gain_of(got, 2 * y + c, 3)).astype(BF)


def assemble(at, mine, other, out):
    core = at[3]
    for c, v in ((core, mine), (1 - core, other)):
        out[pl.ds(pl.multiple_of(c * SEQ, SEQ), SEQ)] = v[...]


def per_device(
    tokens,
    norm_gain,
    value_weight,
    glu_weight,
    conv_kernel,
    conv_gain,
    proj_weight,
    mlp_gain,
    gate_weight,
    up_weight,
    down_weight,
    out_gain,
):
    at = jnp.stack([lax.axis_index(n) for n in ("x", "y", "z", "core")]).astype(jnp.int32)

    sent, a, b = call(
        pack_all,
        [((8, SEQ + EXTRA, 256), BF), ((A_ROWS + SMALL, 128), BF), ((B_ROWS, 128), BF)],
        (at,),
        hbm=(
            tokens,
            norm_gain[None],
            mlp_gain[None],
            conv_gain[None],
            out_gain[None],
            gate_weight.T,
            up_weight.T,
            down_weight,
            value_weight.T,
            glu_weight.T,
            proj_weight,
        ),
        scratch=[
            ((1, 256), F32),
            ((1, 256), F32),
            ((1, 64), F32),
            ((1, 256), F32),
            ((2 * SEQ, 256), BF),
            ((A_ROWS + SMALL, 128), BF),
            ((B_ROWS, 128), BF),
            ((EXTRA, 256), BF),
        ],
        copies=30,
        limit=67043328,
        out_space=pltpu.HBM,
    )
    got = exchange(sent, TP)

    b_near = [z_from(b, k) for k in (1, 2, -1)]
    a_near = [x_from(a, k) for k in (1, 2, -1)]
    a0, row = call(pack_a, [((4, A_ROWS, 128), BF), ((4, SMALL, 128), BF)], (at, a, *a_near))
    b0 = call(pack_b, [((2, B_ROWS, 128), BF)] * 2, (at, b, *b_near))
    a1, a2, a3 = z_from(a0, 1), z_from(a0, 2), z_from(a0, -1)
    b1 = [x_from(b0[0], 1), x_from(b0[1], 1)]
    b3 = [x_from(b0[0], -1), x_from(b0[1], -1)]
    b2 = [x_from(b1[0], 1), x_from(b3[1], -1)]

    vg, proj = call(
        pack_plane,
        [((16, 128, 128), BF), ((16, 64, 128), BF)],
        (at, row, z_from(row, 1), z_from(row, 2), z_from(row, -1)),
    )
    vg_other = swap(vg)
    taps_other = swap(conv_kernel)
    projs = [proj] + [y_from(proj, k) for k in (1, 2, 3)]
    projs += [swap(p) for p in projs]

    (conv,) = call(
        module_in,
        [((SEQ, 128), BF)],
        (at, got, vg, vg_other, conv_kernel, taps_other),
        scratch=[((SEQ + 32, 128), F32)],
        flops=2 * SEQ * 2048 * 256,
    )
    hmid, keep = call(
        module_out,
        [((8, SEQ, 256), BF), ((2, SEQ, 256), F32)],
        (at, got, conv, y_from(conv, 1), y_from(conv, 2), y_from(conv, -1), *projs),
        scratch=[((8, SEQ, 256), F32), ((SEQ, 512), BF)],
        flops=2 * SEQ * 512 * 2048,
    )
    hmid_other = swap(hmid)

    gates, acc_b, down = call(
        near,
        [((2 * SEQ, FF), F32), ((2 * SEQ, FF), F32), ((16, FF, 128), BF)],
        (at, hmid, hmid_other),
        hbm=(a0, a1, a3, a2, *b0, *b1, *b3),
        scratch=[
            ((FF, 2048), BF),
            ((FF, 1536), BF),
            ((2 * SEQ, 2048), BF),
            ((2 * SEQ, 1536), BF),
        ],
        flops=2 * 512 * (2048 + 1536) * FF,
        copies=40,
    )
    quarters = [((4, SEQ, 256), BF)] * 2
    mine, other, hidden, down = call(
        far,
        [*quarters, ((2 * SEQ, FF), BF), ((16, FF, 128), BF)],
        (at, hmid, hmid_other, gates, acc_b, down),
        hbm=b2,
        scratch=[((FF, 512), BF), ((2 * SEQ, 512), BF)],
        flops=2 * 512 * FF * (1024 + 512),
        copies=8,
        alias={5: 3},
    )
    mine_rest, other_rest = call(rest, quarters, (at, hidden, down), flops=2 * 512 * FF * 1024)
    halves = [((2, SEQ, 256), BF)] * 2
    part_2, part_1 = call(chip_sum, halves, (at, mine, swap(other)))
    part_3, part_0 = call(chip_sum, halves, (at, mine_rest, swap(other_rest)))
    parts = [y_from(p, k) for k, p in ((1, part_1), (2, part_2), (3, part_3))]
    second, stats = call(
        residual, [((2, SEQ, 256), F32), ((8, SEQ), F32)], (at, keep, part_0, *parts)
    )
    kept, given = call(
        finish,
        [((SEQ, 256), BF), ((SEQ, 256), BF)],
        (at, got, second, stats, *(y_from(stats, k) for k in (1, 2, 3))),
    )
    (out,) = call(assemble, [((2 * SEQ, 256), BF)], (at, kept, swap(given)))
    return out


def solution(mesh):
    split = Mesh(mesh.devices.reshape(2, 4, 4, 4, 2), ("rep", "z", "x", "y", "core"))
    rows, fs, tp = ("rep", "z", "x"), ("z", "x"), ("y", "core")
    in_specs = (
        P(rows, tp),
        P(tp),
        P(fs, tp),
        P(fs, tp),
        P(None, tp),
        P(tp),
        P(fs, tp),
        P(tp),
        P(fs, tp),
        P(fs, tp),
        P(tp, fs),
        P(tp),
    )
    return jax.shard_map(
        per_device, mesh=split, in_specs=in_specs, out_specs=P(rows, tp), check_vma=False
    )
```

```python
import functools

import jax
import jax.numpy as jnp
from jax import lax
from jax.experimental import pallas as pl
from jax.experimental.pallas import tpu as pltpu
from jax.sharding import Mesh
from jax.sharding import PartitionSpec as P


EPS = 1e-05
Z = ("rep", "z")
TP = ("y", "core")
BF = jnp.bfloat16
F32 = jnp.float32
SEQ = 256
TAPS = 31
FF, SMALL = 704, 192
DA, DB = 96, 608
A_ROWS, B_ROWS = FF + DA, FF + DB
EXTRA = 16


def call(body, outs, args, scratch=(), flops=0, hbm=(), copies=0, limit=None, out_space=pltpu.VMEM, alias=None):
    size = sum(a.size * a.dtype.itemsize for a in args) + sum(
        functools.reduce(lambda p, q: p * q, s, 1) * jnp.dtype(d).itemsize for s, d in outs
    )
    held = sum(
        functools.reduce(lambda p, q: p * q, s, 1) * jnp.dtype(d).itemsize for s, d in scratch
    )
    return pl.pallas_call(
        body,
        out_shape=[jax.ShapeDtypeStruct(s, d) for s, d in outs],
        in_specs=[pl.BlockSpec(memory_space=pltpu.SMEM)]
        + [pl.BlockSpec(memory_space=pltpu.VMEM)] * (len(args) - 1)
        + [pl.BlockSpec(memory_space=pltpu.HBM)] * len(hbm),
        out_specs=[pl.BlockSpec(memory_space=out_space)] * len(outs),
        scratch_shapes=[pltpu.VMEM(s, d) for s, d in scratch]
        + ([pltpu.SemaphoreType.DMA((copies,))] if copies else []),
        compiler_params=pltpu.CompilerParams(vmem_limit_bytes=limit or size + held + (6 << 20)),
        cost_estimate=pl.CostEstimate(
            flops=max(flops, size * 10), bytes_accessed=size, transcendentals=0
        ),
        input_output_aliases=alias or {},
    )(*args, *hbm)


def ring(x, axes, step, size):
    return lax.ppermute(x, axes, [((i + step) % size, i) for i in range(size)])


def y_from(x, step):
    return ring(x, "y", step, 4)


def x_from(x, step):
    return ring(x, "x", step, 4)


def z_from(x, step):
    if step == 2:
        return lax.ppermute(x, Z, [((i + (2 if i % 2 == 0 else -2)) % 8, i) for i in range(8)])
    return ring(x, Z, step, 8)


def swap(x):
    return lax.ppermute(x, "core", [(0, 1), (1, 0)])


def exchange(x, axes):
    return lax.all_to_all(x, axes, 0, 0, tiled=True)


class Copies:
    def __init__(self, sems):
        self.sems, self.count = sems, 0

    def start(self, src, dst):
        copy = pltpu.make_async_copy(src, dst, self.sems.at[self.count])
        self.count += 1
        copy.start()
        return copy


def dot(a, b):
    return jnp.dot(a, b, preferred_element_type=F32)


def dot_t(a, b):
    return lax.dot_general(a, b, (((1,), (1,)), ((), ())), preferred_element_type=F32)


def for_units(body):
    @pl.loop(0, 2)
    def _(j):
        body(pl.ds(pl.multiple_of(j * 256, 256), 256))

    body(pl.ds(512, FF - 512))


def silu(v):
    return v * jax.nn.sigmoid(v)


def pack_all(at, tokens, g0, g1, g2, g3, gate, up, down, value, glu, proj, sent, a, b, *refs):
    norm_gain, mlp_gain, conv_gain, out_gain, rows, packed_a, packed_b, params, sems = refs
    copies = Copies(sems)
    into_b = [
        copies.start(up, packed_b.at[pl.ds(0, FF)]),
        copies.start(down.at[pl.ds(DA, DB)], packed_b.at[pl.ds(FF, DB)]),
    ]
    into_a = [
        copies.start(src, packed_a.at[pl.ds(first, count)])
        for src, first, count in (
            (gate, 0, FF),
            (down.at[pl.ds(0, DA)], FF, DA),
            (value, A_ROWS, 64),
            (glu, A_ROWS + 64, 64),
            (proj.at[:, pl.ds(0, 128)], A_ROWS + 128, 32),
            (proj.at[:, pl.ds(128, 128)], A_ROWS + 160, 32),
        )
    ]
    pairs = ((g0, norm_gain), (g1, mlp_gain), (g2, conv_gain), (g3, out_gain))
    gains = [copies.start(src, dst) for src, dst in pairs]
    into_rows = copies.start(tokens, rows)
    for copy in into_b:
        copy.wait()
    out = [copies.start(packed_b, b)]
    for copy in into_a:
        copy.wait()
    out.append(copies.start(packed_a, a))
    into_rows.wait()
    for t in range(8):
        out.append(copies.start(rows.at[pl.ds(t % 2 * SEQ, SEQ)], sent.at[t, pl.ds(0, SEQ)]))
    for copy in gains:
        copy.wait()
    row = lax.broadcasted_iota(jnp.int32, (EXTRA, 256), 0)
    extra = jnp.zeros((EXTRA, 256), F32)
    wide = jnp.concatenate([conv_gain[...], jnp.zeros((1, 192), F32)], axis=1)
    for i, g in enumerate((norm_gain[...], mlp_gain[...], wide, out_gain[...])):
        high = g.astype(BF).astype(F32)
        mid = (g - high).astype(BF).astype(F32)
        low = g - high - mid
        for j, part in enumerate((high, mid, low)):
            extra = jnp.where(row == 3 * i + j, part, extra)
    params[...] = extra.astype(BF)
    for t in range(8):
        out.append(copies.start(params, sent.at[t, pl.ds(SEQ, EXTRA)]))
    for copy in out:
        copy.wait()


def gain_of(got, t, i):
    rows = got[t, SEQ:].astype(F32)
    return rows[3 * i : 3 * i + 1] + rows[3 * i + 1 : 3 * i + 2] + rows[3 * i + 2 : 3 * i + 3]


def pack_a(at, p0, p1, p2, p3, out, small):
    for k, p in enumerate((p0, p1, p2, p3)):
        i = (at[0] + k) % 4
        out[i] = p[0:A_ROWS]
        small[i] = p[A_ROWS:]


def pack_b(at, p0, p1, p2, p3, low, high):
    for k, p in enumerate((p0, p1, p2, p3)):
        i = (at[2] + k) % 4

        @pl.when(i < 2)
        def _():
            low[i] = p[...]

        @pl.when(i >= 2)
        def _():
            high[i - 2] = p[...]


def pack_plane(at, s0, s1, s2, s3, vg, proj):
    for k, s in enumerate((s0, s1, s2, s3)):
        zz = (at[2] + k) % 4
        for i in range(4):
            vg[zz * 4 + i] = s[i, 0:128]
            proj[zz * 4 + i] = s[i, 128:192]


def module_in(at, got, vg, vg_other, taps, taps_other, out, padded):
    core = at[3]
    total = jnp.zeros((SEQ, 1), F32)
    for t in range(8):
        total = total + jnp.sum(got[t, 0:SEQ].astype(F32), axis=1, keepdims=True)
    mean = total / 2048
    total = jnp.zeros((SEQ, 1), F32)
    for t in range(8):
        off = got[t, 0:SEQ].astype(F32) - mean
        total = total + jnp.sum(off * off, axis=1, keepdims=True)
    scale = lax.rsqrt(total / 2048 + EPS)

    def step(t, acc):
        hin = ((got[t, 0:SEQ].astype(F32) - mean) * scale * gain_of(got, t, 0)).astype(BF)
        w = jnp.concatenate(
            [jnp.concatenate([v[2 * t], v[2 * t + 1]], axis=1) for v in (vg, vg_other)], axis=0
        )
        return acc + dot_t(hin, w)

    acc = lax.fori_loop(0, 8, step, jnp.zeros((SEQ, 256), F32), unroll=4)
    both = acc.astype(BF).astype(F32)
    lane = lax.broadcasted_iota(jnp.int32, (SEQ, 128), 1)

    def gated(v):
        return v * jax.nn.sigmoid(pltpu.roll(v, 64, 1))

    mine, other = gated(both[:, 0:128]), gated(both[:, 128:256])
    is0 = core == 0
    unit = jnp.where(
        lane < 64,
        jnp.where(is0, mine, other),
        pltpu.roll(jnp.where(is0, other, mine), 64, 1),
    )
    padded[0:32] = jnp.zeros((32, 128), F32)
    padded[32:] = unit
    ta, tb = taps[...].astype(F32), taps_other[...].astype(F32)
    first, second = jnp.where(is0, ta, tb), jnp.where(is0, tb, ta)
    k = jnp.concatenate([first, second], axis=1)
    conv = jnp.zeros((SEQ, 128), F32)
    for s in range(TAPS):
        conv = conv + k[s : s + 1] * padded[32 - s : 32 - s + SEQ]
    out[...] = conv.astype(BF)


def module_out(at, got, c0, c1, c2, c3, *refs):
    y, core = at[1], at[3]
    conv = (c0, c1, c2, c3)
    hmid, keep, first, mixed = refs[8:]
    total = jnp.zeros((SEQ, 1), F32)
    for k in range(4):
        total = total + jnp.sum(conv[k][...].astype(F32), axis=1, keepdims=True)
    mean = total / 512
    total = jnp.zeros((SEQ, 1), F32)
    for k in range(4):
        off = conv[k][...].astype(F32) - mean
        total = total + jnp.sum(off * off, axis=1, keepdims=True)
    scale = lax.rsqrt(total / 512 + EPS)
    for k in range(4):
        t = (y + k) % 4
        gain = jnp.concatenate(
            [gain_of(got, 2 * t, 2)[:, 0:64], gain_of(got, 2 * t + 1, 2)[:, 0:64]], axis=1
        )
        mixed[:, pl.ds(pl.multiple_of(t * 128, 128), 128)] = silu(
            (conv[k][...].astype(F32) - mean) * scale * gain
        ).astype(BF)

    total = jnp.zeros((SEQ, 1), F32)
    for k in range(4):
        t = (y + k) % 4
        for p, c in ((refs[k], core), (refs[4 + k], 1 - core)):
            w = jnp.concatenate(
                [p[:, 0:32].reshape(512, 128), p[:, 32:64].reshape(512, 128)], axis=1
            )
            block = got[2 * t + c, 0:SEQ].astype(F32) + dot(mixed[...], w)
            first[2 * t + c] = block
            total = total + jnp.sum(block, axis=1, keepdims=True)
    mean = total / 2048
    total = jnp.zeros((SEQ, 1), F32)
    for t in range(8):
        off = first[t] - mean
        total = total + jnp.sum(off * off, axis=1, keepdims=True)
    scale = lax.rsqrt(total / 2048 + EPS)
    for t in range(8):
        hmid[t] = ((first[t] - mean) * scale * gain_of(got, t, 1)).astype(BF)
    for i in range(2):
        keep[i] = first[2 * y + i]


def lay_a(h0, h1, ha, z):
    for row, h in ((0, h0), (SEQ, h1)):
        for n, k in enumerate((0, 1, 3, 2)):
            for p in range(2):
                c = (4 * n + 2 * p) * 128
                ha[row : row + SEQ, c : c + 256] = h[2 * ((z + k) % 4) + p]


def lay_b(h0, h1, hb, x, steps):
    for row, h in ((0, h0), (SEQ, h1)):
        for n, k in enumerate(steps):
            xx = (x + k) % 4
            lane = pl.ds(pl.multiple_of((xx % 2) * 128, 128), 128)
            for i in range(4):
                c = (4 * n + i) * 128
                hb[row : row + SEQ, c : c + 128] = h[2 * i + xx // 2, :, lane]


def fetch_b(copies, pieces, wb):
    return [
        copies.start(p.at[i, pl.ds(0, FF)], wb.at[:, pl.ds((2 * n + i) * 128, 128)])
        for n, p in enumerate(pieces)
        for i in range(2)
    ]


def fetch_down(copies, pieces, steps, x, down):
    return [
        copies.start(
            pieces[2 * n + p].at[i, pl.ds(FF, DB)],
            down.at[(2 * p + i) * 4 + (x + k) % 4, pl.ds(DA, DB)],
        )
        for n, k in enumerate(steps)
        for p in range(2)
        for i in range(2)
    ]


def near(at, h0, h1, a0, a1, a3, a2, *refs):
    gates, acc_b, down, wa, wb, ha, hb, sems = refs[6:]
    x, z = at[0], at[2]
    copies = Copies(sems)
    into_b = fetch_b(copies, refs[:6], wb)
    into_a = [
        copies.start(p.at[i, pl.ds(0, FF)], wa.at[:, pl.ds((4 * n + i) * 128, 128)])
        for n, p in enumerate((a0, a1, a3, a2))
        for i in range(4)
    ]
    into_down = fetch_down(copies, refs[:6], (0, 1, 3), x, down) + [
        copies.start(p.at[i, pl.ds(FF, DA)], down.at[(z + k) % 4 * 4 + i, pl.ds(0, DA)])
        for k, p in ((0, a0), (1, a1), (3, a3), (2, a2))
        for i in range(4)
    ]
    lay_b(h0, h1, hb, x, (0, 1, 3))
    lay_a(h0, h1, ha, z)
    for copy in into_b:
        copy.wait()

    @for_units
    def _(units):
        acc_b[:, units] = dot_t(hb[...], wb[units])

    for copy in into_a:
        copy.wait()

    @for_units
    def _(units):
        gates[:, units] = silu(dot_t(ha[...], wa[units]))

    for copy in into_down:
        copy.wait()


def products(hidden, down, mine, other, chip, stride):
    @pl.loop(0, 2)
    def _(j):
        for i in range(2):
            t = 2 * ((chip + stride * j) % 4) + i
            right = jnp.concatenate([down[2 * t], down[2 * t + 1]], axis=1)
            res = dot(hidden[...], right).astype(BF)
            mine[2 * j + i] = res[0:SEQ]
            other[2 * j + i] = res[SEQ:]


def far(at, h0, h1, gates, acc_b, down_in, b2l, b2h, mine, other, hidden, down, wb, hb, sems):
    x, y = at[0], at[1]
    copies = Copies(sems)
    into_b = fetch_b(copies, (b2l, b2h), wb)
    into_down = fetch_down(copies, (b2l, b2h), (2,), x, down)
    lay_b(h0, h1, hb, x, (2,))
    for copy in into_b:
        copy.wait()

    @for_units
    def _(units):
        ups = acc_b[:, units] + dot_t(hb[...], wb[units])
        hidden[:, units] = (gates[:, units] * ups).astype(BF)

    for copy in into_down:
        copy.wait()
    products(hidden, down, mine, other, y + 2, 1)


def rest(at, hidden, down, mine, other):
    products(hidden, down, mine, other, at[1] + 1, 3)


def chip_sum(at, mine, got, *outs):
    for j in range(2):
        for i in range(2):
            t = 2 * j + i
            outs[j][i] = (mine[t].astype(F32) + got[t].astype(F32)).astype(BF)


def residual(at, keep, p0, p1, p2, p3, second, stats):
    lane = lax.broadcasted_iota(jnp.int32, (SEQ, 128), 1)
    s0 = jnp.zeros((SEQ, 1), F32)
    s1 = jnp.zeros((SEQ, 1), F32)
    for i in range(2):
        v = keep[i]
        for p in (p0, p1, p2, p3):
            v = v + p[i].astype(F32)
        second[i] = v
        s0 = s0 + jnp.sum(v, axis=1, keepdims=True)
        s1 = s1 + jnp.sum(v * v, axis=1, keepdims=True)
    stats[...] = jnp.where(lane == 0, s0, jnp.where(lane == 1, s1, 0.0)).T[0:8]


def finish(at, got, second, s0, s1, s2, s3, keep, give):
    y, core = at[1], at[3]
    total = s0[...] + s1[...] + s2[...] + s3[...]
    cols = jnp.concatenate([total, jnp.zeros((120, SEQ), F32)], axis=0).T
    mean = cols[:, 0:1] / 2048
    var = cols[:, 1:2] / 2048 - mean * mean
    scale = lax.rsqrt(var + EPS)
    for out, c in ((keep, core), (give, 1 - core)):
        out[...] = ((second[c] - mean) * scale * gain_of(got, 2 * y + c, 3)).astype(BF)


def assemble(at, mine, other, out):
    core = at[3]
    for c, v in ((core, mine), (1 - core, other)):
        out[pl.ds(pl.multiple_of(c * SEQ, SEQ), SEQ)] = v[...]


def per_device(
    tokens,
    norm_gain,
    value_weight,
    glu_weight,
    conv_kernel,
    conv_gain,
    proj_weight,
    mlp_gain,
    gate_weight,
    up_weight,
    down_weight,
    out_gain,
):
    at = jnp.stack([lax.axis_index(n) for n in ("x", "y", "z", "core")]).astype(jnp.int32)

    sent, a, b = call(
        pack_all,
        [((8, SEQ + EXTRA, 256), BF), ((A_ROWS + SMALL, 128), BF), ((B_ROWS, 128), BF)],
        (at,),
        hbm=(
            tokens,
            norm_gain[None],
            mlp_gain[None],
            conv_gain[None],
            out_gain[None],
            gate_weight.T,
            up_weight.T,
            down_weight,
            value_weight.T,
            glu_weight.T,
            proj_weight,
        ),
        scratch=[
            ((1, 256), F32),
            ((1, 256), F32),
            ((1, 64), F32),
            ((1, 256), F32),
            ((2 * SEQ, 256), BF),
            ((A_ROWS + SMALL, 128), BF),
            ((B_ROWS, 128), BF),
            ((EXTRA, 256), BF),
        ],
        copies=31,
        limit=67043328,
        out_space=pltpu.HBM,
    )
    got = exchange(sent, TP)

    b_near = [z_from(b, k) for k in (1, 2, -1)]
    a_near = [x_from(a, k) for k in (1, 2, -1)]
    a0, row = call(pack_a, [((4, A_ROWS, 128), BF), ((4, SMALL, 128), BF)], (at, a, *a_near))
    b0 = call(pack_b, [((2, B_ROWS, 128), BF)] * 2, (at, b, *b_near))
    a1, a2, a3 = z_from(a0, 1), z_from(a0, 2), z_from(a0, -1)
    b1 = [x_from(b0[0], 1), x_from(b0[1], 1)]
    b3 = [x_from(b0[0], -1), x_from(b0[1], -1)]
    b2 = [x_from(b1[0], 1), x_from(b3[1], -1)]

    vg, proj = call(
        pack_plane,
        [((16, 128, 128), BF), ((16, 64, 128), BF)],
        (at, row, z_from(row, 1), z_from(row, 2), z_from(row, -1)),
    )
    vg_other = swap(vg)
    taps_other = swap(conv_kernel)
    projs = [proj] + [y_from(proj, k) for k in (1, 2, 3)]
    projs += [swap(p) for p in projs]

    (conv,) = call(
        module_in,
        [((SEQ, 128), BF)],
        (at, got, vg, vg_other, conv_kernel, taps_other),
        scratch=[((SEQ + 32, 128), F32)],
        flops=2 * SEQ * 2048 * 256,
    )
    hmid, keep = call(
        module_out,
        [((8, SEQ, 256), BF), ((2, SEQ, 256), F32)],
        (at, got, conv, y_from(conv, 1), y_from(conv, 2), y_from(conv, -1), *projs),
        scratch=[((8, SEQ, 256), F32), ((SEQ, 512), BF)],
        flops=2 * SEQ * 512 * 2048,
    )
    hmid_other = swap(hmid)

    gates, acc_b, down = call(
        near,
        [((2 * SEQ, FF), F32), ((2 * SEQ, FF), F32), ((16, FF, 128), BF)],
        (at, hmid, hmid_other),
        hbm=(a0, a1, a3, a2, *b0, *b1, *b3),
        scratch=[
            ((FF, 2048), BF),
            ((FF, 1536), BF),
            ((2 * SEQ, 2048), BF),
            ((2 * SEQ, 1536), BF),
        ],
        flops=2 * 512 * (2048 + 1536) * FF,
        copies=56,
    )
    quarters = [((4, SEQ, 256), BF)] * 2
    mine, other, hidden, down = call(
        far,
        [*quarters, ((2 * SEQ, FF), BF), ((16, FF, 128), BF)],
        (at, hmid, hmid_other, gates, acc_b, down),
        hbm=b2,
        scratch=[((FF, 512), BF), ((2 * SEQ, 512), BF)],
        flops=2 * 512 * FF * (1024 + 512),
        copies=8,
        alias={5: 3},
    )
    mine_rest, other_rest = call(rest, quarters, (at, hidden, down), flops=2 * 512 * FF * 1024)
    halves = [((2, SEQ, 256), BF)] * 2
    part_2, part_1 = call(chip_sum, halves, (at, mine, swap(other)))
    part_3, part_0 = call(chip_sum, halves, (at, mine_rest, swap(other_rest)))
    parts = [y_from(p, k) for k, p in ((1, part_1), (2, part_2), (3, part_3))]
    second, stats = call(
        residual, [((2, SEQ, 256), F32), ((8, SEQ), F32)], (at, keep, part_0, *parts)
    )
    kept, given = call(
        finish,
        [((SEQ, 256), BF), ((SEQ, 256), BF)],
        (at, got, second, stats, *(y_from(stats, k) for k in (1, 2, 3))),
    )
    (out,) = call(assemble, [((2 * SEQ, 256), BF)], (at, kept, swap(given)))
    return out


def solution(mesh):
    split = Mesh(mesh.devices.reshape(2, 4, 4, 4, 2), ("rep", "z", "x", "y", "core"))
    rows, fs, tp = ("rep", "z", "x"), ("z", "x"), ("y", "core")
    in_specs = (
        P(rows, tp),
        P(tp),
        P(fs, tp),
        P(fs, tp),
        P(None, tp),
        P(tp),
        P(fs, tp),
        P(tp),
        P(fs, tp),
        P(fs, tp),
        P(tp, fs),
        P(tp),
    )
    return jax.shard_map(
        per_device, mesh=split, in_specs=in_specs, out_specs=P(rows, tp), check_vma=False
    )
```
